32 devices in a mesh: rep: 2 (over x), fs: 8 (over z, y), tp: 2 (over core).
Axes of the slice: x: 2, y: 2, z: 4, core: 2. Of those that a mesh axis runs over, the one named last changes fastest.
Arguments:
- tokens: bfloat16 [8192, 2048], P(('rep', 'fs')), may hold values from -6 to 6
- mixer_gain: float32 [2048], replicated, may hold values from 0.1 to 1.9
- pool_input: float32 [2048, 1024], P('fs', 'tp'), may hold values from -0.125 to 0.125
- input_scale: float32 [1024], P('tp'), may hold values from 0.5 to 2
- group_mix: float32 [128, 1024], P(None, 'tp'), may hold values from -0.5 to 0.5
- group_scale: float32 [1024], P('tp'), may hold values from 0.5 to 2
- pool_output: float32 [2048, 1024], P('fs', 'tp'), may hold values from -0.1875 to 0.1875
- output_scale: float32 [2048], P('fs'), may hold values from 0.5 to 2
- channel_gain: float32 [2048], replicated, may hold values from 0.1 to 1.9
- gate_weight: float32 [2048, 5632], P('fs', 'tp'), may hold values from -0.125 to 0.125
- gate_scale: float32 [5632], P('tp'), may hold values from 0.5 to 2
- up_weight: float32 [2048, 5632], P('fs', 'tp'), may hold values from -0.125 to 0.125
- up_scale: float32 [5632], P('tp'), may hold values from 0.5 to 2
- down_weight: float32 [2048, 5632], P('fs', 'tp'), may hold values from -0.078125 to 0.078125
- down_scale: float32 [2048], P('fs'), may hold values from 0.5 to 2
Outputs:
- layer_out: bfloat16 [8192, 2048], P(('rep', 'fs'))
The draws below stay inside these ranges and needn't reach their ends.
All inputs are finite; a program needn't handle non-finite values.
Results may differ from the reference program's by a relative error of at most 0.02.
Values may be sent and summed in bfloat16 or wider, within the bound.
A program may use at most 128 MiB of HBM per device.

```python
import math
import jax
import jax.numpy as jnp
from jax import lax

D = 2048
FF = 5632
POOL_GROUP = 256
MAP_WIDTH = 128
POOL_WIDTH = 1024
SEQ = 512
TOKENS = 8192
N_TP = 2


def block_levels(stream_key, shape, cuts, smallest, high):
    gain = 1.0
    for dim, parts in cuts:
        draws = jax.random.uniform(jax.random.fold_in(jax.random.fold_in(stream_key, 6), dim), (parts,), jnp.float32, smallest / len(cuts), high / len(cuts))
        gain = gain * jnp.repeat(jnp.exp(draws), shape[dim] // parts).reshape((-1,) + (1,) * (len(shape) - 1 - dim))
    return gain


def normal_values(stream_key, extent, width, bound, shards=(), kind=jnp.bfloat16):
    entries = width * jax.random.normal(stream_key, extent, jnp.float32)
    if shards:
        entries = entries * block_levels(stream_key, extent, shards, -0.22, 0.18)
    return jnp.clip(entries, -bound, bound).astype(kind)


def setup_inputs(seed: int = 0) -> dict:
    key_list = jax.random.split(jax.random.key(seed), 16)
    return {
        "tokens": normal_values(key_list[0], (TOKENS, D), 1.0, 6.0, ((0, 16),)),
        "mixer_gain": jnp.clip(1.0 + 0.18 * jax.random.normal(key_list[1], (D,), jnp.float32), 0.1, 1.9),
        "pool_input": normal_values(key_list[2], (D, POOL_WIDTH), D ** -0.5, 0.125, ((0, 8), (1, 2)), jnp.float32),
        "input_scale": jnp.clip(jnp.exp(math.log(2.0) - 1.3862944 * jax.random.uniform(key_list[3], (POOL_WIDTH,), jnp.float32) ** block_levels(key_list[3], (POOL_WIDTH,), ((0, 2),), -0.2, 0.2)), 0.5, 2.0),
        "group_mix": normal_values(key_list[4], (MAP_WIDTH, POOL_WIDTH), MAP_WIDTH ** -0.5, 0.5, ((1, 2),), jnp.float32),
        "group_scale": jnp.clip(jnp.exp(math.log(2.0) - 1.3862944 * jax.random.uniform(key_list[5], (POOL_WIDTH,), jnp.float32) ** block_levels(key_list[5], (POOL_WIDTH,), ((0, 2),), -0.2, 0.2)), 0.5, 2.0),
        "pool_output": normal_values(key_list[6], (D, POOL_WIDTH), POOL_WIDTH ** -0.5, 0.1875, ((0, 8), (1, 2)), jnp.float32),
        "output_scale": jnp.clip(jnp.exp(math.log(2.0) - 1.3862944 * jax.random.uniform(key_list[7], (D,), jnp.float32) ** block_levels(key_list[7], (D,), ((0, 8),), -0.2, 0.2)), 0.5, 2.0),
        "channel_gain": jnp.clip(1.0 + 0.18 * jax.random.normal(key_list[8], (D,), jnp.float32), 0.1, 1.9),
        "gate_weight": normal_values(key_list[9], (D, FF), D ** -0.5, 0.125, ((0, 8), (1, 2)), jnp.float32),
        "gate_scale": jnp.clip(jnp.exp(math.log(2.0) - 1.3862944 * jax.random.uniform(key_list[10], (FF,), jnp.float32) ** block_levels(key_list[10], (FF,), ((0, 2),), -0.2, 0.2)), 0.5, 2.0),
        "up_weight": normal_values(key_list[11], (D, FF), D ** -0.5, 0.125, ((0, 8), (1, 2)), jnp.float32),
        "up_scale": jnp.clip(jnp.exp(math.log(2.0) - 1.3862944 * jax.random.uniform(key_list[12], (FF,), jnp.float32) ** block_levels(key_list[12], (FF,), ((0, 2),), -0.2, 0.2)), 0.5, 2.0),
        "down_weight": normal_values(key_list[13], (D, FF), FF ** -0.5, 0.078125, ((0, 8), (1, 2)), jnp.float32),
        "down_scale": jnp.clip(jnp.exp(math.log(2.0) - 1.3862944 * jax.random.uniform(key_list[14], (D,), jnp.float32) ** block_levels(key_list[14], (D,), ((0, 8),), -0.2, 0.2)), 0.5, 2.0),
    }


epsilon = 1e-06

def rms_norm(row_block, gain_row):
    floats = row_block.astype(jnp.float32)
    scaled = floats * lax.rsqrt(lax.optimization_barrier(jnp.mean(floats * floats, axis=-1, keepdims=True)) + epsilon)
    return (scaled * gain_row).astype(jnp.bfloat16)

def block_sum(left_rows, weight_rows, feature_scale, blocks):
    length = left_rows.shape[0]
    block_width = left_rows.shape[1] // blocks
    left_split = left_rows.astype(jnp.float32).reshape(length, blocks, block_width)
    right_split = weight_rows.astype(jnp.bfloat16).astype(jnp.float32).reshape(weight_rows.shape[0], blocks, block_width)
    partials = jnp.einsum('sjc,djc->jsd', left_split, right_split)
    rounded = (partials * feature_scale).astype(jnp.bfloat16)
    rounded = lax.optimization_barrier(rounded)
    return lax.optimization_barrier(jnp.sum(rounded.astype(jnp.float32), axis=0))

def one_layer(row_block, mixer_gain, pool_input, input_scale, group_mix, group_scale, pool_output, output_scale, channel_gain, gate_weight, gate_scale, up_weight, up_scale, down_weight, down_scale):
    length = row_block.shape[0]
    normed = rms_norm(row_block, mixer_gain)
    pool_in = (jnp.dot(normed, pool_input.astype(jnp.bfloat16), preferred_element_type=jnp.float32) * input_scale).astype(jnp.bfloat16)
    grouped_in = pool_in.astype(jnp.float32).reshape(length, 4, POOL_GROUP)
    running = jnp.concatenate([jnp.zeros((1, 4, POOL_GROUP), jnp.float32), jnp.cumsum(grouped_in, axis=0)], axis=0)
    places = jnp.arange(length, dtype=jnp.int32)
    window_means = []
    for group_index in range(4):
        window = 2 ** (group_index + 1)
        first_row = jnp.maximum(places + 1 - window, 0).astype(jnp.int32)
        counts = (places + 1 - first_row).astype(jnp.float32)
        window_sum = running[1:, group_index] - running[first_row, group_index]
        window_means.append(window_sum / counts[:, None] - grouped_in[:, group_index])
    pooled = jnp.stack(window_means, axis=1).astype(jnp.bfloat16).reshape(length, POOL_WIDTH)
    map_blocks = POOL_WIDTH // MAP_WIDTH
    mix_matrix = group_mix.astype(jnp.bfloat16).astype(jnp.float32).reshape(MAP_WIDTH, map_blocks, MAP_WIDTH)
    mixed_raw = jnp.einsum('sgc,cgd->sgd', pooled.astype(jnp.float32).reshape(length, map_blocks, MAP_WIDTH), mix_matrix).reshape(length, POOL_WIDTH)
    grouped = (mixed_raw * group_scale).astype(jnp.bfloat16)
    mixer_out = block_sum(grouped, pool_output, output_scale, N_TP)
    middle = (row_block.astype(jnp.float32) + mixer_out).astype(jnp.bfloat16)
    second = rms_norm(middle, channel_gain)
    gate_sum = jnp.dot(second, gate_weight.astype(jnp.bfloat16), preferred_element_type=jnp.float32) * gate_scale
    up_sum = jnp.dot(second, up_weight.astype(jnp.bfloat16), preferred_element_type=jnp.float32) * up_scale
    hidden = (jax.nn.silu(gate_sum) * up_sum).astype(jnp.bfloat16)
    channel_out = block_sum(hidden, down_weight, down_scale, N_TP)
    return (middle.astype(jnp.float32) + channel_out).astype(jnp.bfloat16)

def reference(tokens, mixer_gain, pool_input, input_scale, group_mix, group_scale, pool_output, output_scale, channel_gain, gate_weight, gate_scale, up_weight, up_scale, down_weight, down_scale):
    sequences = tokens.reshape(TOKENS // SEQ, SEQ, D)

    def each_sequence(row_block):
        return one_layer(row_block, mixer_gain, pool_input, input_scale, group_mix, group_scale, pool_output, output_scale, channel_gain, gate_weight, gate_scale, up_weight, up_scale, down_weight, down_scale)
    results = lax.map(each_sequence, sequences)
    return results.reshape(TOKENS, D)
```

```python
import jax
import jax.numpy as jnp
from jax import lax
from jax.sharding import PartitionSpec as P

POOL_GROUP = 256

epsilon = 1e-06


def normed_rows(floats, gain_row):
    scaled = floats * lax.rsqrt(jnp.mean(floats * floats, axis=-1, keepdims=True) + epsilon)
    return (scaled * gain_row).astype(jnp.bfloat16)


def product(left_rows, weight):
    return jnp.dot(left_rows, weight, preferred_element_type=jnp.float32)


def transposed_product(left_rows, weight_rows):
    return lax.dot_general(
        left_rows, weight_rows, (((1,), (1,)), ((), ())), preferred_element_type=jnp.float32
    )


def thirds(scale):
    high = lax.reduce_precision(scale, 8, 7)
    rest = scale - high
    middle = lax.reduce_precision(rest, 8, 7)
    return [piece.astype(jnp.bfloat16) for piece in (high, middle, rest - middle)]


def make_body(reps, shards, cores):
    def over_rep(value):
        return lax.ppermute(value, "rep", [(i, (i + 1) % reps) for i in range(reps)])

    def over_pair(value):
        return lax.ppermute(value, "fs", [(i, i ^ 1) for i in range(shards)])

    def sum_cores(value):
        if cores == 2:
            core = lax.axis_index("tp")
            rows = value.shape[0] // 2
            other = lax.dynamic_slice_in_dim(value, (1 - core) * rows, rows, 0)
            own = lax.dynamic_slice_in_dim(value, core * rows, rows, 0)
            other = lax.ppermute(other.astype(jnp.bfloat16), "tp", [(0, 1), (1, 0)])
            own = lax.optimization_barrier(own.astype(jnp.bfloat16))
            return own.astype(jnp.float32) + other.astype(jnp.float32)
        total = lax.psum_scatter(
            value.astype(jnp.bfloat16), "tp", scatter_dimension=0, tiled=True
        )
        return total.astype(jnp.float32)

    def gather_cores(value):
        if cores == 2:
            core = lax.axis_index("tp")
            other = lax.ppermute(value, "tp", [(0, 1), (1, 0)])
            first = jnp.where(core == 0, value, other)
            second = jnp.where(core == 0, other, value)
            return jnp.concatenate([first, second], axis=0)
        return lax.all_gather(value, "tp", axis=0, tiled=True)

    lines = [[i for i in range(shards) if i % 2 == side] for side in range(2)]

    def body(
        tokens,
        mixer_gain,
        pool_input,
        input_scale,
        group_mix,
        group_scale,
        pool_output,
        output_scale,
        channel_gain,
        gate_weight,
        gate_scale,
        up_weight,
        up_scale,
        down_weight,
        down_scale,
    ):
        rep = lax.axis_index("rep")
        side = lax.axis_index("fs") % 2
        core = lax.axis_index("tp")
        length = tokens.shape[0]
        block_width = group_mix.shape[0]
        local_width = group_mix.shape[1]
        half_width = local_width // 2

        start = rep * half_width
        halves = [
            lax.dynamic_slice_in_dim(weight, start, half_width, 1).astype(jnp.bfloat16)
            for weight in (pool_input, pool_output)
        ]
        columns = jnp.stack(thirds(output_scale) + thirds(down_scale), axis=1)
        columns = jnp.pad(columns, ((0, 0), (0, 128 - columns.shape[1])))
        mine = lax.all_gather(
            jnp.concatenate(halves + [columns], axis=1), "fs", axis=0, tiled=True
        )
        feature = mine[:, local_width : local_width + 6].astype(jnp.float32).T
        output_feature = feature[0:1] + feature[1:2] + feature[2:3]
        down_feature = feature[3:4] + feature[4:5] + feature[5:6]
        mine = mine[:, :local_width]
        theirs = over_rep(mine)
        first = jnp.where(rep == 0, mine, theirs)
        second_half = jnp.where(rep == 0, theirs, mine)
        input_full = jnp.concatenate([first[:, :half_width], second_half[:, :half_width]], axis=1)
        output_full = jnp.concatenate([first[:, half_width:], second_half[:, half_width:]], axis=1)

        share = gate_weight.shape[1] // (2 * reps)

        def cut(weight, which):
            return lax.dynamic_slice_in_dim(
                weight, (rep * 2 + which) * share, share, weight.ndim - 1
            )

        def paired(weights):
            keep = jnp.concatenate([cut(w, side).astype(jnp.bfloat16) for w in weights], axis=1)
            send = jnp.concatenate([cut(w, 1 - side).astype(jnp.bfloat16) for w in weights], axis=1)
            came = over_pair(send)
            low = jnp.where(side == 0, keep, came)
            high = jnp.where(side == 0, came, keep)
            block = jnp.concatenate([low, high], axis=0)
            return lax.all_gather(block, "fs", axis=0, tiled=True, axis_index_groups=lines)

        gate_up = paired((gate_weight, up_weight))
        down_full = paired((down_weight,))

        normed = normed_rows(tokens.astype(jnp.float32), mixer_gain)
        pool_in = (product(normed, input_full) * input_scale).astype(jnp.bfloat16)
        places = jnp.arange(length, dtype=jnp.int32)
        offsets = places[:, None] - places[None, :]
        channel_group = (
            core * local_width + jnp.arange(local_width, dtype=jnp.int32)
        ) // POOL_GROUP
        pooled_mean = jnp.zeros((length, local_width), jnp.float32)
        for group_index in range(4):
            window = 2 ** (group_index + 1)
            band_mask = ((offsets >= 0) & (offsets < window)).astype(jnp.bfloat16)
            window_sums = product(band_mask, pool_in)
            counts = jnp.minimum(places + 1, window).astype(jnp.float32)
            pooled_mean = jnp.where(
                channel_group[None, :] == group_index, window_sums / counts[:, None], pooled_mean
            )
        pooled = (pooled_mean - pool_in.astype(jnp.float32)).astype(jnp.bfloat16)
        local_blocks = local_width // block_width
        mixed_raw = jnp.einsum(
            "sgc,cgd->sgd",
            pooled.reshape(length, local_blocks, block_width),
            group_mix.astype(jnp.bfloat16).reshape(block_width, local_blocks, block_width),
            preferred_element_type=jnp.float32,
        ).reshape(length, local_width)
        grouped = (mixed_raw * group_scale).astype(jnp.bfloat16)
        mixer_out = sum_cores(transposed_product(grouped, output_full) * output_feature)

        rows = length // cores
        own_tokens = lax.dynamic_slice_in_dim(tokens, core * rows, rows, 0)
        middle = (own_tokens.astype(jnp.float32) + mixer_out).astype(jnp.bfloat16)
        middle = lax.optimization_barrier(middle)
        second = normed_rows(middle.astype(jnp.float32), channel_gain)

        from_rep = over_rep(second)
        from_side = over_pair(second)
        half_rows = rows // 2
        corner = jnp.concatenate(
            [over_pair(from_rep[:half_rows]), over_rep(from_side[half_rows:])], axis=0
        )
        member_rows = jnp.concatenate([second, from_rep, from_side, corner], axis=0)
        group_rows = gather_cores(member_rows)

        width = share
        both = product(group_rows, gate_up)
        gate_sum = both[:, :width] * cut(gate_scale, side)
        up_sum = both[:, width:] * cut(up_scale, side)
        hidden = (jax.nn.silu(gate_sum) * up_sum).astype(jnp.bfloat16)
        partial = sum_cores(transposed_product(hidden, down_full))
        partial = partial.astype(jnp.bfloat16).reshape(4, rows, -1)
        half = partial.shape[2] // 2
        left, right = partial[:, :, :half], partial[:, :, half:]

        def added(one, two):
            return (one.astype(jnp.float32) + two.astype(jnp.float32)).astype(jnp.bfloat16)

        left_came = over_rep(left[1::2])
        right_came = over_pair(right[2:])
        left_two = left[0::2].astype(jnp.float32) + left_came.astype(jnp.float32)
        right_two = right[:2].astype(jnp.float32) + right_came.astype(jnp.float32)
        left_last = over_pair(left_two[1].astype(jnp.bfloat16)).astype(jnp.float32)
        right_last = over_rep(right_two[1].astype(jnp.bfloat16)).astype(jnp.float32)
        total = jnp.concatenate([left_two[0] + left_last, right_two[0] + right_last], axis=1)
        own_out = (middle.astype(jnp.float32) + total * down_feature).astype(jnp.bfloat16)
        return gather_cores(own_out)

    return body


def solution(mesh):
    in_specs = (
        P(("rep", "fs"), None),
        P(),
        P("fs", "tp"),
        P("tp"),
        P(None, "tp"),
        P("tp"),
        P("fs", "tp"),
        P("fs"),
        P(),
        P("fs", "tp"),
        P("tp"),
        P("fs", "tp"),
        P("tp"),
        P("fs", "tp"),
        P("fs"),
    )
    out_specs = P(("rep", "fs"), None)
    body = make_body(mesh.shape["rep"], mesh.shape["fs"], mesh.shape["tp"])
    return jax.shard_map(body, mesh=mesh, in_specs=in_specs, out_specs=out_specs, check_vma=False)
```

```python
import jax
import jax.numpy as jnp
from jax import lax
from jax.sharding import PartitionSpec as P

POOL_GROUP = 256

epsilon = 1e-06


def normed_rows(floats, gain_row):
    scaled = floats * lax.rsqrt(jnp.mean(floats * floats, axis=-1, keepdims=True) + epsilon)
    return (scaled * gain_row).astype(jnp.bfloat16)


def product(left_rows, weight):
    return jnp.dot(left_rows, weight, preferred_element_type=jnp.float32)


def transposed_product(left_rows, weight_rows):
    return lax.dot_general(
        left_rows, weight_rows, (((1,), (1,)), ((), ())), preferred_element_type=jnp.float32
    )


def thirds(scale):
    high = lax.reduce_precision(scale, 8, 7)
    rest = scale - high
    middle = lax.reduce_precision(rest, 8, 7)
    return [piece.astype(jnp.bfloat16) for piece in (high, middle, rest - middle)]


def make_body(reps, shards, cores):
    def over_rep(value):
        return lax.ppermute(value, "rep", [(i, (i + 1) % reps) for i in range(reps)])

    def over_pair(value):
        return lax.ppermute(value, "fs", [(i, i ^ 1) for i in range(shards)])

    def over_cores(value):
        return lax.ppermute(value, "tp", [(0, 1), (1, 0)])

    def sum_cores(value):
        if cores == 2:
            core = lax.axis_index("tp")
            rows = value.shape[0] // 2
            other = lax.dynamic_slice_in_dim(value, (1 - core) * rows, rows, 0)
            own = lax.dynamic_slice_in_dim(value, core * rows, rows, 0)
            other = lax.ppermute(other.astype(jnp.bfloat16), "tp", [(0, 1), (1, 0)])
            own = lax.optimization_barrier(own.astype(jnp.bfloat16))
            return own.astype(jnp.float32) + other.astype(jnp.float32)
        total = lax.psum_scatter(
            value.astype(jnp.bfloat16), "tp", scatter_dimension=0, tiled=True
        )
        return total.astype(jnp.float32)

    def gather_cores(value):
        if cores == 2:
            core = lax.axis_index("tp")
            other = lax.ppermute(value, "tp", [(0, 1), (1, 0)])
            first = jnp.where(core == 0, value, other)
            second = jnp.where(core == 0, other, value)
            return jnp.concatenate([first, second], axis=0)
        return lax.all_gather(value, "tp", axis=0, tiled=True)

    lines = [[i for i in range(shards) if i % 2 == side] for side in range(2)]

    def body(
        tokens,
        mixer_gain,
        pool_input,
        input_scale,
        group_mix,
        group_scale,
        pool_output,
        output_scale,
        channel_gain,
        gate_weight,
        gate_scale,
        up_weight,
        up_scale,
        down_weight,
        down_scale,
    ):
        rep = lax.axis_index("rep")
        side = lax.axis_index("fs") % 2
        core = lax.axis_index("tp")
        length = tokens.shape[0]
        block_width = group_mix.shape[0]
        local_width = group_mix.shape[1]

        def arranged(own, peer):
            low = jnp.where(side == 0, own, peer)
            high = jnp.where(side == 0, peer, own)
            return low, high

        def share_of(weight, which):
            share = weight.shape[-1] // (2 * reps)
            return lax.dynamic_slice_in_dim(
                weight, (rep * 2 + which) * share, share, weight.ndim - 1
            )

        def shares(weights, which):
            return [share_of(weight, which).astype(jnp.bfloat16) for weight in weights]

        def along_line(block):
            return lax.all_gather(block, "fs", axis=0, tiled=True, axis_index_groups=lines)

        columns = jnp.stack(thirds(output_scale) + thirds(down_scale), axis=1)
        columns = jnp.pad(columns, ((0, 0), (0, 128 - columns.shape[1])))
        mixer_weights = (pool_input, pool_output)
        keep = jnp.concatenate(shares(mixer_weights, side) + [columns], axis=1)
        send = jnp.concatenate(shares(mixer_weights, 1 - side) + [columns], axis=1)
        mine = along_line(jnp.concatenate(arranged(keep, over_pair(send)), axis=0))

        channel_weights = (gate_weight, up_weight, down_weight)
        keep = jnp.concatenate(shares(channel_weights, side), axis=1)
        send = jnp.concatenate(shares(channel_weights, 1 - side), axis=1)
        low, high = arranged(keep, over_pair(send))
        width = keep.shape[1] // 3
        block = jnp.concatenate([low[:, : 2 * width], high[:, : 2 * width]], axis=0)
        block, low, high, mine = lax.optimization_barrier(
            (block, low[:, 2 * width :], high[:, 2 * width :], mine)
        )
        gate_up = along_line(block)
        down_parts = [along_line(low), along_line(high)]

        quarter = local_width // 4
        feature = mine[:, 2 * quarter : 2 * quarter + 6].astype(jnp.float32).T
        output_feature = feature[0:1] + feature[1:2] + feature[2:3]
        down_feature = feature[3:4] + feature[4:5] + feature[5:6]
        mine = mine[:, : 2 * quarter]
        by_rep = over_rep(mine)
        by_side = over_pair(mine)
        split = mine.shape[0] // 2
        by_both = jnp.concatenate([over_pair(by_rep[:split]), over_rep(by_side[split:])], axis=0)
        own_low, own_high = arranged(mine, by_side)
        peer_low, peer_high = arranged(by_rep, by_both)
        quarters = [
            jnp.where(rep == 0, own_low, peer_low),
            jnp.where(rep == 0, own_high, peer_high),
            jnp.where(rep == 0, peer_low, own_low),
            jnp.where(rep == 0, peer_high, own_high),
        ]
        input_full = jnp.concatenate([piece[:, :quarter] for piece in quarters], axis=1)
        output_full = jnp.concatenate([piece[:, quarter:] for piece in quarters], axis=1)

        normed = normed_rows(tokens.astype(jnp.float32), mixer_gain)
        pool_in = (product(normed, input_full) * input_scale).astype(jnp.bfloat16)
        places = jnp.arange(length, dtype=jnp.int32)
        window_sums = pool_in.astype(jnp.float32)
        channel_group = (
            core * local_width + jnp.arange(local_width, dtype=jnp.int32)
        ) // POOL_GROUP
        pooled_mean = jnp.zeros((length, local_width), jnp.float32)
        for group_index in range(4):
            window = 2 ** (group_index + 1)
            shift = window // 2
            window_sums = window_sums + jnp.pad(window_sums[:-shift], ((shift, 0), (0, 0)))
            counts = jnp.minimum(places + 1, window).astype(jnp.float32)
            pooled_mean = jnp.where(
                channel_group[None, :] == group_index, window_sums / counts[:, None], pooled_mean
            )
        pooled = (pooled_mean - pool_in.astype(jnp.float32)).astype(jnp.bfloat16)
        local_blocks = local_width // block_width
        mixed_raw = jnp.einsum(
            "sgc,cgd->sgd",
            pooled.reshape(length, local_blocks, block_width),
            group_mix.astype(jnp.bfloat16).reshape(block_width, local_blocks, block_width),
            preferred_element_type=jnp.float32,
        ).reshape(length, local_width)
        grouped = (mixed_raw * group_scale).astype(jnp.bfloat16)
        mixer_out = sum_cores(transposed_product(grouped, output_full) * output_feature)

        rows = length // cores
        own_tokens = lax.dynamic_slice_in_dim(tokens, core * rows, rows, 0)
        middle = (own_tokens.astype(jnp.float32) + mixer_out).astype(jnp.bfloat16)
        middle = lax.optimization_barrier(middle)
        second = normed_rows(middle.astype(jnp.float32), channel_gain)

        from_rep = over_rep(second)
        from_side = over_pair(second)
        half_rows = rows // 2
        corner = jnp.concatenate(
            [over_pair(from_rep[:half_rows]), over_rep(from_side[half_rows:])], axis=0
        )
        member_rows = jnp.concatenate([second, from_rep, from_side, corner], axis=0)
        if cores == 2:
            row_sets = [over_cores(member_rows), member_rows]
        else:
            row_sets = [lax.all_gather(member_rows, "tp", axis=0, tiled=True)]

        def activated(row_set):
            both = product(row_set, gate_up)
            gate_sum = both[:, :width] * share_of(gate_scale, side)
            up_sum = both[:, width:] * share_of(up_scale, side)
            return (jax.nn.silu(gate_sum) * up_sum).astype(jnp.bfloat16)

        hidden_sets = lax.optimization_barrier([activated(row_set) for row_set in row_sets])

        def wide(value):
            return value.astype(jnp.float32)

        def scattered(down_part, hidden_sets):
            partials = [
                transposed_product(hidden, down_part).astype(jnp.bfloat16)
                for hidden in hidden_sets
            ]
            if cores == 2:
                summed = wide(over_cores(partials[0])) + wide(partials[1])
            else:
                summed = wide(
                    lax.psum_scatter(partials[0], "tp", scatter_dimension=0, tiled=True)
                )
            partial = summed.astype(jnp.bfloat16).reshape(4, rows, -1)
            half = partial.shape[2] // 2
            left, right = partial[:, :, :half], partial[:, :, half:]
            left_two = wide(left[0::2]) + wide(over_rep(left[1::2]))
            right_two = wide(right[:2]) + wide(over_pair(right[2:]))
            left_last = wide(over_pair(left_two[1].astype(jnp.bfloat16)))
            right_last = wide(over_rep(right_two[1].astype(jnp.bfloat16)))
            total = jnp.concatenate([left_two[0] + left_last, right_two[0] + right_last], axis=1)
            return total.reshape(rows, shards // 2, -1)

        low_total = scattered(down_parts[0], hidden_sets)
        low_total, hidden_sets = lax.optimization_barrier((low_total, hidden_sets))
        high_total = scattered(down_parts[1], hidden_sets)
        total = jnp.stack([low_total, high_total], axis=2)
        total = total.reshape(rows, -1)
        own_out = (middle.astype(jnp.float32) + total * down_feature).astype(jnp.bfloat16)
        return gather_cores(own_out)

    return body


def solution(mesh):
    in_specs = (
        P(("rep", "fs"), None),
        P(),
        P("fs", "tp"),
        P("tp"),
        P(None, "tp"),
        P("tp"),
        P("fs", "tp"),
        P("fs"),
        P(),
        P("fs", "tp"),
        P("tp"),
        P("fs", "tp"),
        P("tp"),
        P("fs", "tp"),
        P("fs"),
    )
    out_specs = P(("rep", "fs"), None)
    body = make_body(mesh.shape["rep"], mesh.shape["fs"], mesh.shape["tp"])
    return jax.shard_map(body, mesh=mesh, in_specs=in_specs, out_specs=out_specs, check_vma=False)
```
